256 devices in a mesh: ep: 64 (over z, x, core), tp: 4 (over y).
Axes of the slice: x: 4, y: 4, z: 8, core: 2. Of those that a mesh axis runs over, the one named last changes fastest.
Arguments:
- tokens_a: bfloat16 [16384, 2048], P('ep', 'tp'), may hold values from -60 to 60
- norm_gain_a: float32 [2048], P('tp'), may hold values from 0.1 to 1.9
- pool_weight: bfloat16 [4, 512, 512], P('tp'), may hold values from -0.25 to 0.25
- pool_scale: float32 [2048], P('tp'), may hold values from 0.1 to 1.9
- tokens_b: bfloat16 [16384, 2048], P('ep'), may hold values from -6 to 6
- norm_gain_b: float32 [2048], replicated, may hold values from 0.1 to 1.9
- routes: int32 [16384, 2], P('ep'), may hold values from 0 to 63, all different within a row; in each aligned block of 256 rows (0 to 255, 256 to 511, ...) at most 12 rows name the same one
- route_logits: float32 [16384, 2], P('ep'), may hold values from -4 to 4
- expert_gate: bfloat16 [64, 2048, 3584], P('ep', None, 'tp'), may hold values from -0.125 to 0.125
- expert_up: bfloat16 [64, 2048, 3584], P('ep', None, 'tp'), may hold values from -0.125 to 0.125
- expert_down: bfloat16 [64, 3584, 2048], P('ep', 'tp'), may hold values from -0.09375 to 0.09375
Outputs:
- mixed_a: bfloat16 [16384, 2048], P('ep', 'tp')
- moe_out: bfloat16 [16384, 2048], P('ep', 'tp')
The draws below stay inside these ranges and needn't reach their ends.
Inputs may be any that keep to these rules, and one draw needn't show every extreme that they name: `routes`: among the 256 rows of one index of ep, at most 12 rows name any one expert, a bound that some block reaches.
All inputs are finite; a program needn't handle non-finite values.
Results may differ from the reference program's by a relative error of at most 0.012.
Values may be sent and summed in bfloat16 or wider, within the bound.
No kernel may reach another device: no remote copies, remote signals or barrier semaphores. Data moves between devices by JAX's collectives and lax.ppermute only.
A program may use at most 128 MiB of HBM per device.

```python
import math
import jax
import jax.numpy as jnp
import numpy as np
from jax import lax

D = 2048
GROUPS = 4
GC = 512
FF = 3584
FF_PART = 896
TOP = 2
TOK_DEV = 256
TOKENS = 16384
EXPERTS = 64
CAP = 12
N_EP = 64
N_TP = 4


def draw_tokens_a(key, part):
    column = jnp.arange(D, dtype=jnp.float32) / D
    column_scale = jnp.exp(jnp.log(10.0) * column)
    base = jnp.clip(jax.random.normal(key, (TOKENS, D), jnp.float32), -6.0, 6.0)
    return (base * column_scale[None, :]).astype(jnp.bfloat16)


def shard_levels(own_key, dims, pieces, smallest, top_value):
    level, own = 1.0, jax.random.fold_in(own_key, 6)
    for axis_at, parts in pieces:
        steps = jnp.exp(jax.random.uniform(jax.random.fold_in(own, axis_at), (parts,), jnp.float32, smallest / len(pieces), top_value / len(pieces)))
        level = level * jnp.repeat(steps, dims[axis_at] // parts).reshape([-1 if axis == axis_at else 1 for axis in range(len(dims))])
    return level


def assign_block(stream_key, own, number, rows, amount, top, limit, skew):
    ranking = jax.random.permutation(stream_key, amount)
    packed, common = portions_of(amount, rows * top, limit, skew, True), portions_of(amount, rows * top, limit, skew, False)
    places = jnp.arange(amount)

    def named(lengths, rotation):
        used = int((lengths > 0).sum())
        fixed = max(1, used // 4)
        passed = fixed + (places - fixed + rotation * (used - fixed)) % max(1, amount - fixed)
        return jnp.zeros((amount,), jnp.int32).at[ranking[jnp.where(places < fixed, places, passed)]].set(jnp.asarray(lengths, jnp.int32))

    lengths = jnp.where(number % 4 == 0, named(packed, number // 4), named(common, number - number // 4 - 1))
    mixed = jax.random.permutation(jax.random.fold_in(own, 3), amount)
    donor, taker = mixed[0:amount // 2 * 2:2], mixed[1:amount // 2 * 2:2]
    margin = jnp.minimum(lengths[donor] - 1, limit - lengths[taker]) // 2
    margin = jnp.where((donor == ranking[0]) | (taker == ranking[0]) | (lengths[taker] == 0), 0, jnp.maximum(margin, 0))
    passed = jax.random.randint(jax.random.fold_in(own, 4), (amount // 2,), 0, 1 << 20) % (margin + 1)
    lengths = lengths.at[donor].add(-passed).at[taker].add(passed)
    members = jnp.searchsorted(jnp.cumsum(lengths), jnp.arange(rows * top), side="right").astype(jnp.int32)
    table = members.reshape(top, rows).T
    table = table[jax.random.permutation(jax.random.fold_in(own, 1), rows)]
    rotation = jax.random.randint(jax.random.fold_in(own, 2), (rows, 1), 0, top)
    return jnp.take_along_axis(table, (jnp.arange(top)[None, :] + rotation) % top, axis=1)


def portions_of(amount, total, bound, skew, full):
    loads = [(1 << 20) // math.isqrt(standing ** skew) + 1 for standing in range(1, amount + 1)]
    largest = bound if full else min(bound, max(-(-total // amount), total * loads[0] // sum(loads)))
    least = 1 if total - largest >= amount - 1 else 0
    holding, rest = [largest] + [least] * (amount - 1), total - largest - least * (amount - 1)
    while rest > 0:
        movable = [i for i in range(1, amount) if holding[i] < largest] or [i for i in range(1, amount) if holding[i] < bound]
        whole, remaining = sum([loads[i] for i in movable]), rest
        for i in movable:
            more = min(bound - holding[i], max(1, remaining * loads[i] // whole), rest)
            holding[i] = holding[i] + more
            rest = rest - more
    return np.array(holding)


def centred(stream_key, shape, width, limit, pieces=(), kind=jnp.bfloat16):
    values = jax.random.normal(stream_key, shape, jnp.float32) * width
    if len(pieces) > 0:
        values = shard_levels(stream_key, shape, pieces, -0.22, 0.18) * values
    return jnp.clip(values, min=-limit, max=limit).astype(kind)


def setup_inputs(seed: int = 0) -> dict:
    arg_keys = jax.random.split(jax.random.key(seed), 12)
    tokens_a = draw_tokens_a(jax.random.fold_in(arg_keys[11], 71), 0)
    norm_gain_a = jnp.clip(1.0 + 0.18 * jax.random.normal(arg_keys[1], (D,), jnp.float32), 0.1, 1.9)
    pool_weight = centred(arg_keys[2], (GROUPS, GC, GC), GC ** -0.5, 0.25, ((0, 4),))
    pool_scale = jnp.clip(1.0 + 0.18 * jax.random.normal(arg_keys[3], (D,), jnp.float32), 0.1, 1.9)
    tokens_b = centred(arg_keys[4], (TOKENS, D), 1.0, 6.0, ((0, 64),))
    norm_gain_b = jnp.clip(1.0 + 0.18 * jax.random.normal(arg_keys[5], (D,), jnp.float32), 0.1, 1.9)
    routes_keys = jax.random.split(jax.random.fold_in(arg_keys[6], 1), TOKENS // TOK_DEV)
    routes_turns = jax.random.permutation(jax.random.fold_in(arg_keys[6], 3), TOKENS // TOK_DEV)
    routes = jax.vmap(lambda own, number: assign_block(jax.random.fold_in(arg_keys[6], 2), own, number, TOK_DEV, EXPERTS, TOP, CAP, 1))(routes_keys, routes_turns).reshape((TOKENS, TOP))
    route_logits = centred(arg_keys[7], (TOKENS, TOP), 1.0, 4.0, ((0, 64),), jnp.float32)
    expert_gate = centred(arg_keys[8], (EXPERTS, D, FF), D ** -0.5, 0.125, ((0, 64), (2, 4)))
    expert_up = centred(arg_keys[9], (EXPERTS, D, FF), D ** -0.5, 0.125, ((0, 64), (2, 4)))
    expert_down = centred(arg_keys[10], (EXPERTS, FF, D), FF ** -0.5, 0.09375, ((0, 64), (1, 4)))
    return dict(tokens_a=tokens_a, norm_gain_a=norm_gain_a, pool_weight=pool_weight, pool_scale=pool_scale, tokens_b=tokens_b, norm_gain_b=norm_gain_b, routes=routes, route_logits=route_logits, expert_gate=expert_gate, expert_up=expert_up, expert_down=expert_down)


epsilon = 1e-06

def rms_norm(values, scale_gain):
    floats = values.astype(jnp.float32)
    scaled = floats * lax.rsqrt(lax.optimization_barrier(jnp.mean(floats * floats, axis=-1, keepdims=True)) + epsilon)
    return (scaled * scale_gain.astype(jnp.float32)).astype(jnp.bfloat16)

def reference(tokens_a, norm_gain_a, pool_weight, pool_scale, tokens_b, norm_gain_b, routes, route_logits, expert_gate, expert_up, expert_down):
    normed_a = rms_norm(tokens_a, norm_gain_a).astype(jnp.float32)
    position = jnp.arange(1, TOKENS + 1, dtype=jnp.float32)[:, None]
    outputs = []
    for group_index in range(GROUPS):
        window = 2 ** (group_index + 1)
        column = normed_a[:, group_index * GC:(group_index + 1) * GC]
        padded = jnp.pad(column, ((window - 1, 0), (0, 0)))
        pooled = jnp.zeros_like(column)
        for offset in range(window):
            begin_row = window - 1 - offset
            pooled = pooled + padded[begin_row:begin_row + TOKENS]
        pooled = pooled / jnp.minimum(position, jnp.float32(window))
        difference = (pooled - column).astype(jnp.bfloat16)
        product = jnp.dot(difference, pool_weight[group_index], preferred_element_type=jnp.float32)
        outputs.append((product * pool_scale[group_index * GC:(group_index + 1) * GC]).astype(jnp.bfloat16))
    mixed_a = jnp.concatenate(outputs, axis=1)
    normed_b = rms_norm(tokens_b, norm_gain_b)
    logit_exp = jnp.exp(route_logits)
    route_weight = logit_exp / lax.optimization_barrier(jnp.sum(logit_exp, axis=1, keepdims=True))
    flat_expert = routes.reshape(-1).astype(jnp.int32)
    onehot = (flat_expert[:, None] == jnp.arange(EXPERTS, dtype=jnp.int32)[None, :]).astype(jnp.int32)
    blocked = onehot.reshape(N_EP, TOK_DEV * TOP, EXPERTS)
    earlier = (jnp.cumsum(blocked, axis=1) - blocked).reshape(TOKENS * TOP, EXPERTS)
    position_in = lax.optimization_barrier(jnp.sum(earlier * onehot, axis=1)).astype(jnp.int32)
    source = jnp.arange(TOKENS * TOP, dtype=jnp.int32) // (TOK_DEV * TOP)
    slot_count = N_EP * CAP
    slot_index = flat_expert * slot_count + source * CAP + position_in
    token_of = jnp.arange(TOKENS * TOP, dtype=jnp.int32) // TOP
    slot_token = jnp.full((EXPERTS * slot_count,), TOKENS, jnp.int32).at[slot_index].set(token_of)
    slot_weight = jnp.zeros((EXPERTS * slot_count,), jnp.float32).at[slot_index].set(route_weight.reshape(-1))

    def expert_step(accumulated, inputs):
        gate_weight, up_weight, down_weight, chosen, weight = inputs
        row_block = jnp.take(normed_b, chosen, axis=0, mode='fill', fill_value=0)
        gate_part = jnp.dot(row_block, gate_weight, preferred_element_type=jnp.float32)
        up_part = jnp.dot(row_block, up_weight, preferred_element_type=jnp.float32)
        hidden = (jax.nn.silu(gate_part) * up_part).astype(jnp.bfloat16)
        result = jnp.zeros((slot_count, D), jnp.float32)
        for part_index in range(N_TP):
            lower = part_index * FF_PART
            piece = jnp.dot(hidden[:, lower:lower + FF_PART], down_weight[lower:lower + FF_PART], preferred_element_type=jnp.float32)
            rounded = lax.optimization_barrier(piece.astype(jnp.bfloat16))
            result = result + rounded.astype(jnp.float32)
        accumulated = accumulated.at[chosen].add(result * weight[:, None], mode='drop')
        return (accumulated, None)
    accumulated, _ = lax.scan(expert_step, jnp.zeros((TOKENS, D), jnp.float32), (expert_gate, expert_up, expert_down, slot_token.reshape(EXPERTS, slot_count), slot_weight.reshape(EXPERTS, slot_count)))
    moe_out = accumulated.astype(jnp.bfloat16)
    return (mixed_a, moe_out)
```

```python
import functools

import jax
import jax.numpy as jnp
from jax import lax
from jax.experimental import pallas as pl
from jax.experimental.pallas import tpu as pltpu
from jax.sharding import PartitionSpec as P

D = 2048
EPS = 1e-06
EXPERTS = 64
TOK = 256
GC = 512
FF_PART = 896
HALF = 256
SLOT_ROWS = 24
HALF_EXPERTS = EXPERTS // 2


f32 = jnp.float32
bf16 = jnp.bfloat16


def whole(*names):
    return [pl.BlockSpec(memory_space=n) for n in names]


def dot(a, b):
    return jnp.dot(a, b, preferred_element_type=f32)


def pack_kernel(tp_ref, tokens_ref, gain_ref, routes_ref, out_ref, index_ref):
    share = tp_ref[0]
    x = tokens_ref[...].astype(f32)
    mean = jnp.sum(x * x, axis=1, keepdims=True) / D
    start = pl.multiple_of(share * GC, GC)
    own = tokens_ref[:, pl.ds(start, GC)].astype(f32)
    normed = (own * lax.rsqrt(mean + EPS) * gain_ref[:, pl.ds(start, GC)]).astype(bf16)
    expert_rows = lax.broadcasted_iota(jnp.int32, (EXPERTS, TOK), 0)
    earlier = (
        lax.broadcasted_iota(jnp.int32, (TOK, TOK), 0) < lax.broadcasted_iota(jnp.int32, (TOK, TOK), 1)
    ).astype(f32).astype(bf16)
    first = jnp.zeros((EXPERTS, 1), f32)
    lows, highs = [], []
    for k in range(2):
        chosen = routes_ref[k : k + 1, :]
        onehot = (expert_rows == chosen).astype(f32)
        count = dot(onehot.astype(bf16), earlier) + first
        slot = jnp.sum(onehot * count, axis=0, keepdims=True).astype(jnp.int32)
        first = first + jnp.sum(onehot, axis=1, keepdims=True)
        base = chosen * SLOT_ROWS
        lows.append(base + jnp.where(slot < 8, slot, slot + 8))
        highs.append(base + jnp.where(slot < 8, slot + 8, slot + 12))
    index_ref[...] = jnp.concatenate([*lows, *highs], axis=0)
    rows = lax.broadcasted_iota(jnp.int32, (EXPERTS * SLOT_ROWS, TOK), 0)
    low = jnp.where((rows == lows[0]) | (rows == lows[1]), 1.0, 0.0).astype(bf16)
    high = jnp.where((rows == highs[0]) | (rows == highs[1]), 1.0, 0.0).astype(bf16)
    out_ref[...] = (dot(low, normed[:, :HALF]) + dot(high, normed[:, HALF:])).astype(bf16)


def pack(tp, tokens_b, gain, routes):
    return pl.pallas_call(
        pack_kernel,
        out_shape=(
            jax.ShapeDtypeStruct((EXPERTS * SLOT_ROWS, HALF), bf16),
            jax.ShapeDtypeStruct((4, TOK), jnp.int32),
        ),
        in_specs=whole(pltpu.SMEM, pltpu.VMEM, pltpu.VMEM, pltpu.VMEM),
        out_specs=tuple(whole(pltpu.VMEM, pltpu.VMEM)),
        name="pack",
    )(tp, tokens_b, gain, routes)


HALF_ROWS = HALF_EXPERTS * 12
MAIN = HALF_EXPERTS * 8
MIX = HALF_EXPERTS * 4


def picker(n_out, n_in, group_out, group_in, offset):
    r = lax.broadcasted_iota(jnp.int32, (n_out, n_in), 0)
    c = lax.broadcasted_iota(jnp.int32, (n_out, n_in), 1)
    if group_out < group_in:
        hit = (r // group_out) * group_in + r % group_out + offset == c
    else:
        hit = (c // group_in) * group_out + c % group_in + offset == r
    return hit.astype(f32).astype(bf16)


def rows_of(ref):
    a = ref[...].reshape(HALF_EXPERTS, SLOT_ROWS, HALF)
    main = jnp.concatenate([a[:, 0:8].reshape(MAIN, HALF), a[:, 8:16].reshape(MAIN, HALF)], axis=1)
    mixed = a[:, 16:24].reshape(MAIN, HALF)
    low = dot(picker(MIX, MAIN, 4, 8, 0), mixed).astype(bf16)
    high = dot(picker(MIX, MAIN, 4, 8, 4), mixed).astype(bf16)
    return jnp.concatenate([main, jnp.concatenate([low, high], axis=1)], axis=0)


def store_rows(ref, rows):
    main, mix = rows[:MAIN], rows[MAIN:]
    tail = dot(picker(MAIN, MIX, 8, 4, 0), mix[:, :HALF]) + dot(picker(MAIN, MIX, 8, 4, 4), mix[:, HALF:])
    pieces = [
        main[:, :HALF].reshape(HALF_EXPERTS, 8, HALF),
        main[:, HALF:].reshape(HALF_EXPERTS, 8, HALF),
        tail.astype(bf16).reshape(HALF_EXPERTS, 8, HALF),
    ]
    ref[...] = jnp.concatenate(pieces, axis=1).reshape(HALF_EXPERTS * SLOT_ROWS, HALF)


SHARES = (0, 3, 1, 2)
SLABS = (2, 1, 3, 0)


def expert_kernel(tp_ref, gate_ref, up_ref, down_ref, *refs):
    x_refs, o_refs = refs[:8], refs[8:16]
    gate_w, up_w, down_w, gate_acc, up_acc, gate_sem, up_sem, down_sem = refs[16:]
    tp = tp_ref[0]
    gates, ups, downs = [], [], []
    for i, step in enumerate(SHARES):
        source = pl.ds(pl.multiple_of(((tp + step) % 4) * GC, GC), GC)
        gates.append(pltpu.make_async_copy(gate_ref.at[source], gate_w.at[i], gate_sem.at[i]))
        ups.append(pltpu.make_async_copy(up_ref.at[source], up_w.at[i], up_sem.at[i]))
    for i, step in enumerate(SLABS):
        source = pl.ds(pl.multiple_of(((tp + step) % 4) * GC, GC), GC)
        downs.append(pltpu.make_async_copy(down_ref.at[:, source], down_w.at[i], down_sem.at[i]))
    for g, u in zip(gates, ups):
        g.start()
        u.start()
    for d in downs:
        d.start()
    for i in range(4):
        gates[i].wait()
        ups[i].wait()
        for h in range(2):
            x = rows_of(x_refs[2 * i + h])
            span = pl.ds(h * HALF_ROWS, HALF_ROWS)
            g = dot(x, gate_w[i])
            u = dot(x, up_w[i])
            if i:
                g = gate_acc[span] + g
                u = up_acc[span] + u
            gate_acc[span] = g
            up_acc[span] = u
    hidden = []
    for h in range(2):
        g = gate_acc[pl.ds(h * HALF_ROWS, HALF_ROWS)]
        u = up_acc[pl.ds(h * HALF_ROWS, HALF_ROWS)]
        hidden.append((g / (1.0 + jnp.exp(-g)) * u).astype(bf16))
    for i in range(4):
        downs[i].wait()
        for h in range(2):
            store_rows(o_refs[2 * i + h], dot(hidden[h], down_w[i]).astype(bf16))


def experts(tp, gate, up, down, shares):
    piece = jax.ShapeDtypeStruct((HALF_EXPERTS * SLOT_ROWS, HALF), bf16)
    return pl.pallas_call(
        expert_kernel,
        out_shape=(piece,) * 8,
        in_specs=whole(pltpu.SMEM, pl.ANY, pl.ANY, pl.ANY) + whole(*[pltpu.VMEM] * 8),
        out_specs=tuple(whole(*[pltpu.VMEM] * 8)),
        scratch_shapes=[
            pltpu.VMEM((4, GC, FF_PART), bf16),
            pltpu.VMEM((4, GC, FF_PART), bf16),
            pltpu.VMEM((4, FF_PART, GC), bf16),
            pltpu.VMEM((2 * HALF_ROWS, FF_PART), f32),
            pltpu.VMEM((2 * HALF_ROWS, FF_PART), f32),
            pltpu.SemaphoreType.DMA((4,)),
            pltpu.SemaphoreType.DMA((4,)),
            pltpu.SemaphoreType.DMA((4,)),
        ],
        name="experts",
        compiler_params=pltpu.CompilerParams(vmem_limit_bytes=48 * 1024 * 1024),
    )(tp, gate, up, down, *shares)


def combine_kernel(index_ref, logits_ref, low_ref, out_ref):
    e = jnp.exp(logits_ref[...])
    weight = e / jnp.sum(e, axis=1, keepdims=True)
    columns = lax.broadcasted_iota(jnp.int32, (TOK, EXPERTS * SLOT_ROWS), 1)
    rows = low_ref[...]
    for h in range(2):
        total = None
        for k in range(2):
            at = index_ref[:, 2 * h + k : 2 * h + k + 1]
            pick = jnp.where(columns == at, 1.0, 0.0).astype(bf16)
            term = dot(pick, rows) * weight[:, k : k + 1]
            total = term if total is None else total + term
        out_ref[:, h * HALF : (h + 1) * HALF] = total.astype(bf16)


def combine(index, logits, rows):
    return pl.pallas_call(
        combine_kernel,
        out_shape=jax.ShapeDtypeStruct((TOK, GC), bf16),
        in_specs=whole(*[pltpu.VMEM] * 3),
        out_specs=whole(pltpu.VMEM)[0],
        name="combine",
    )(index, logits, rows)


RIM = 16
EXT = RIM + TOK


def squares_kernel(rim_ref, own_ref, out_ref):
    rim = rim_ref[...].astype(f32)
    own = own_ref[...].astype(f32)
    out_ref[:RIM] = jnp.broadcast_to(jnp.sum(rim * rim, axis=1, keepdims=True), (RIM, 128))
    out_ref[RIM:] = jnp.broadcast_to(jnp.sum(own * own, axis=1, keepdims=True), (TOK, 128))


def mixer_kernel(place_ref, squares_ref, rim_ref, own_ref, gain_ref, weight_ref, scale_ref, out_ref):
    group = place_ref[1]
    rows = jnp.concatenate([rim_ref[...], own_ref[...]], axis=0).astype(f32)
    normed = (rows * lax.rsqrt(squares_ref[...] / D + EPS) * gain_ref[...]).astype(bf16).astype(f32)
    window = normed + pltpu.roll(normed, 1, 0)
    for level in range(1, 4):
        window = window + jnp.where(group >= level, pltpu.roll(window, 2**level, 0), 0.0)
    length = jnp.left_shift(jnp.int32(1), group + 1).astype(f32)
    position = (
        place_ref[0] * TOK + 1 + lax.broadcasted_iota(jnp.int32, (TOK, GC), 0)
    ).astype(f32)
    pooled = window[RIM:] / jnp.minimum(position, length)
    difference = (pooled - normed[RIM:]).astype(bf16)
    out_ref[...] = (dot(difference, weight_ref[...]) * scale_ref[...]).astype(bf16)


def mixer(place, tokens_a, gain, weight, scale):
    peers = lax.axis_size("ep")
    rim = lax.ppermute(tokens_a[TOK - RIM :], "ep", [(i, i + 1) for i in range(peers - 1)])
    squares = pl.pallas_call(
        squares_kernel,
        out_shape=jax.ShapeDtypeStruct((EXT, 128), f32),
        in_specs=whole(*[pltpu.VMEM] * 2),
        out_specs=whole(pltpu.VMEM)[0],
        name="squares",
    )(rim, tokens_a)[:, 0]
    total = squares
    for step in (1, 3, 2):
        total = total + around(squares, step)
    return pl.pallas_call(
        mixer_kernel,
        out_shape=jax.ShapeDtypeStruct((TOK, GC), bf16),
        in_specs=whole(pltpu.SMEM, *[pltpu.VMEM] * 6),
        out_specs=whole(pltpu.VMEM)[0],
        name="mixer",
    )(place, total[:, None], rim, tokens_a, gain, weight, scale)


def around(x, step):
    return lax.ppermute(x, "tp", [(i, (i + step) % 4) for i in range(4)])


def shards(
    tokens_a,
    norm_gain_a,
    pool_weight,
    pool_scale,
    tokens_b,
    norm_gain_b,
    routes,
    route_logits,
    expert_gate,
    expert_up,
    expert_down,
):
    ep = lax.axis_index("ep").astype(jnp.int32)
    tp = lax.axis_index("tp").astype(jnp.int32)
    tp_at = tp[None]
    packed, index = pack(tp_at, tokens_b, norm_gain_b[None, :], routes.T)
    received = lax.all_to_all(
        packed.reshape(EXPERTS, SLOT_ROWS, HALF), "ep", 0, 0, tiled=True
    ).reshape(2, HALF_EXPERTS * SLOT_ROWS, HALF)
    mixed_a = mixer(jnp.stack([ep, tp]), tokens_a, norm_gain_a[None], pool_weight[0], pool_scale[None])
    a, b = received[0], received[1]
    before_a, after_b = around(a, 1), around(b, 3)
    before_b, after_a = around(b, 1), around(a, 3)
    far_a, far_b = around(before_a, 1), around(after_b, 3)
    far1, far2, next1, next2, prev1, prev2, own1, own2 = experts(
        tp_at,
        expert_gate[0],
        expert_up[0],
        expert_down[0],
        (a, b, before_a, before_b, after_a, after_b, far_a, far_b),
    )
    got_far1, got_far2 = around(far1, 1), around(far2, 3)
    from_before2, from_after1 = around(next2, 1), around(prev1, 3)
    plus = lambda *xs: functools.reduce(jnp.add, [x.astype(f32) for x in xs]).astype(bf16)
    from_before1 = around(plus(next1, got_far1), 1)
    from_after2 = around(plus(prev2, got_far2), 3)
    summed = jnp.stack([plus(own1, from_before1, from_after1), plus(own2, from_before2, from_after2)])
    returned = lax.all_to_all(
        summed.reshape(EXPERTS, SLOT_ROWS, HALF), "ep", 0, 0, tiled=True
    ).reshape(EXPERTS * SLOT_ROWS, HALF)
    moe_out = combine(index.T, route_logits, returned)
    return mixed_a, moe_out


def solution(mesh):
    placed = (
        P("ep", "tp"),
        P("tp"),
        P("tp", None, None),
        P("tp"),
        P("ep", None),
        P(),
        P("ep", None),
        P("ep", None),
        P("ep", None, "tp"),
        P("ep", None, "tp"),
        P("ep", "tp", None),
    )
    return jax.shard_map(
        shards,
        mesh=mesh,
        in_specs=placed,
        out_specs=(P("ep", "tp"), P("ep", "tp")),
        check_vma=False,
    )
```

```python
import functools

import jax
import jax.numpy as jnp
from jax import lax
from jax.experimental import pallas as pl
from jax.experimental.pallas import tpu as pltpu
from jax.sharding import PartitionSpec as P

D = 2048
EPS = 1e-06
EXPERTS = 64
TOK = 256
GC = 512
FF_PART = 896
HALF = 256
SLOT_ROWS = 24
HALF_EXPERTS = EXPERTS // 2


f32 = jnp.float32
bf16 = jnp.bfloat16


def whole(*names):
    return [pl.BlockSpec(memory_space=n) for n in names]


def dot(a, b):
    return jnp.dot(a, b, preferred_element_type=f32)


def pack_kernel(tp_ref, tokens_ref, gain_ref, routes_ref, out_ref, index_ref):
    share = tp_ref[0]
    x = tokens_ref[...].astype(f32)
    mean = jnp.sum(x * x, axis=1, keepdims=True) / D
    start = pl.multiple_of(share * GC, GC)
    own = tokens_ref[:, pl.ds(start, GC)].astype(f32)
    normed = (own * lax.rsqrt(mean + EPS) * gain_ref[:, pl.ds(start, GC)]).astype(bf16)
    expert_rows = lax.broadcasted_iota(jnp.int32, (EXPERTS, TOK), 0)
    earlier = (
        lax.broadcasted_iota(jnp.int32, (TOK, TOK), 0) < lax.broadcasted_iota(jnp.int32, (TOK, TOK), 1)
    ).astype(f32).astype(bf16)
    first = jnp.zeros((EXPERTS, 1), f32)
    lows, highs = [], []
    for k in range(2):
        chosen = routes_ref[k : k + 1, :]
        onehot = (expert_rows == chosen).astype(f32)
        count = dot(onehot.astype(bf16), earlier) + first
        slot = jnp.sum(onehot * count, axis=0, keepdims=True).astype(jnp.int32)
        first = first + jnp.sum(onehot, axis=1, keepdims=True)
        base = chosen * SLOT_ROWS
        lows.append(base + jnp.where(slot < 8, slot, slot + 8))
        highs.append(base + jnp.where(slot < 8, slot + 8, slot + 12))
    index_ref[...] = jnp.concatenate([*lows, *highs], axis=0)
    rows = lax.broadcasted_iota(jnp.int32, (EXPERTS * SLOT_ROWS, TOK), 0)
    low = jnp.where((rows == lows[0]) | (rows == lows[1]), 1.0, 0.0).astype(bf16)
    high = jnp.where((rows == highs[0]) | (rows == highs[1]), 1.0, 0.0).astype(bf16)
    out_ref[...] = (dot(low, normed[:, :HALF]) + dot(high, normed[:, HALF:])).astype(bf16)


def pack(tp, tokens_b, gain, routes):
    return pl.pallas_call(
        pack_kernel,
        out_shape=(
            jax.ShapeDtypeStruct((EXPERTS * SLOT_ROWS, HALF), bf16),
            jax.ShapeDtypeStruct((4, TOK), jnp.int32),
        ),
        in_specs=whole(pltpu.SMEM, pltpu.VMEM, pltpu.VMEM, pltpu.VMEM),
        out_specs=tuple(whole(pltpu.VMEM, pltpu.VMEM)),
        name="pack",
        compiler_params=params(24),
    )(tp, tokens_b, gain, routes)


HALF_ROWS = HALF_EXPERTS * 12
MAIN = HALF_EXPERTS * 8
MIX = HALF_EXPERTS * 4


def picker(n_out, n_in, group_out, group_in, offset):
    r = lax.broadcasted_iota(jnp.int32, (n_out, n_in), 0)
    c = lax.broadcasted_iota(jnp.int32, (n_out, n_in), 1)
    if group_out < group_in:
        hit = (r // group_out) * group_in + r % group_out + offset == c
    else:
        hit = (c // group_in) * group_out + c % group_in + offset == r
    return hit.astype(f32).astype(bf16)


def rows_of(ref):
    a = ref[...].reshape(HALF_EXPERTS, SLOT_ROWS, HALF)
    main = jnp.concatenate([a[:, 0:8].reshape(MAIN, HALF), a[:, 8:16].reshape(MAIN, HALF)], axis=1)
    mixed = a[:, 16:24].reshape(MAIN, HALF)
    low = dot(picker(MIX, MAIN, 4, 8, 0), mixed).astype(bf16)
    high = dot(picker(MIX, MAIN, 4, 8, 4), mixed).astype(bf16)
    return jnp.concatenate([main, jnp.concatenate([low, high], axis=1)], axis=0)


def store_rows(ref, rows):
    main, mix = rows[:MAIN], rows[MAIN:]
    tail = dot(picker(MAIN, MIX, 8, 4, 0), mix[:, :HALF]) + dot(picker(MAIN, MIX, 8, 4, 4), mix[:, HALF:])
    pieces = [
        main[:, :HALF].reshape(HALF_EXPERTS, 8, HALF),
        main[:, HALF:].reshape(HALF_EXPERTS, 8, HALF),
        tail.astype(bf16).reshape(HALF_EXPERTS, 8, HALF),
    ]
    ref[...] = jnp.concatenate(pieces, axis=1).reshape(HALF_EXPERTS * SLOT_ROWS, HALF)


def params(mib):
    return pltpu.CompilerParams(vmem_limit_bytes=mib * 1024 * 1024)


def cost(flops):
    return pl.CostEstimate(flops=int(flops), bytes_accessed=1 << 20, transcendentals=0)


PIECE = jax.ShapeDtypeStruct((HALF_EXPERTS * SLOT_ROWS, HALF), bf16)
ACC = jax.ShapeDtypeStruct((2 * HALF_ROWS, FF_PART), f32)


def half_span(h):
    return pl.ds(h * HALF_ROWS, HALF_ROWS)


def slab(tp_ref, step):
    return pl.ds(pl.multiple_of(((tp_ref[0] + step) % 4) * GC, GC), GC)


def own_share_kernel(tp_ref, gate_ref, up_ref, x0_ref, x1_ref, gate_acc, up_acc):
    at = slab(tp_ref, 0)
    for h, x_ref in enumerate((x0_ref, x1_ref)):
        x = rows_of(x_ref)
        gate_acc[half_span(h)] = dot(x, gate_ref[at, :])
        up_acc[half_span(h)] = dot(x, up_ref[at, :])


def own_share(*args):
    return pl.pallas_call(
        own_share_kernel,
        out_shape=(ACC,) * 2,
        in_specs=whole(pltpu.SMEM, *[pltpu.VMEM] * 4),
        out_specs=tuple(whole(*[pltpu.VMEM] * 2)),
        name="own_share",
        compiler_params=params(24),
        cost_estimate=cost(5e9),
    )(*args)


def near_share_kernel(tp_ref, gate_ref, up_ref, gate_in, up_in, x00, x01, x10, x11, gate_acc, up_acc):
    before, after = slab(tp_ref, 3), slab(tp_ref, 1)
    for h, (xa, xb) in enumerate(((x00, x10), (x01, x11))):
        a, b = rows_of(xa), rows_of(xb)
        span = half_span(h)
        gate_acc[span] = gate_in[span] + (dot(a, gate_ref[before, :]) + dot(b, gate_ref[after, :]))
        up_acc[span] = up_in[span] + (dot(a, up_ref[before, :]) + dot(b, up_ref[after, :]))


def near_share(*args):
    return pl.pallas_call(
        near_share_kernel,
        out_shape=(ACC,) * 2,
        in_specs=whole(pltpu.SMEM, *[pltpu.VMEM] * 8),
        out_specs=tuple(whole(*[pltpu.VMEM] * 2)),
        input_output_aliases={3: 0, 4: 1},
        name="near_share",
        compiler_params=params(24),
        cost_estimate=cost(5e9),
    )(*args)


def far_share_kernel(tp_ref, gate_ref, up_ref, gate_in, up_in, x0, x1, hidden_ref):
    at = slab(tp_ref, 2)
    for h, x_ref in enumerate((x0, x1)):
        x = rows_of(x_ref)
        span = half_span(h)
        g = gate_in[span] + dot(x, gate_ref[at, :])
        u = up_in[span] + dot(x, up_ref[at, :])
        hidden_ref[span] = (g / (1.0 + jnp.exp(-g)) * u).astype(bf16)


def far_share(*args):
    return pl.pallas_call(
        far_share_kernel,
        out_shape=jax.ShapeDtypeStruct((2 * HALF_ROWS, FF_PART), bf16),
        in_specs=whole(pltpu.SMEM, *[pltpu.VMEM] * 6),
        out_specs=whole(pltpu.VMEM)[0],
        name="far_share",
        compiler_params=params(24),
        cost_estimate=cost(5e9),
    )(*args)


def down_kernel(steps, tp_ref, hidden_ref, down_ref, *out_refs):
    for i, step in enumerate(steps):
        weight = down_ref[:, slab(tp_ref, step)]
        for h in range(2):
            store_rows(out_refs[2 * i + h], dot(hidden_ref[half_span(h)], weight).astype(bf16))


def down(name, steps, tp, hidden, weight):
    n = len(steps)
    return pl.pallas_call(
        functools.partial(down_kernel, steps),
        out_shape=(PIECE,) * (2 * n),
        in_specs=whole(pltpu.SMEM, *[pltpu.VMEM] * 2),
        out_specs=tuple(whole(*[pltpu.VMEM] * (2 * n))),
        name=name,
        compiler_params=params(16),
        cost_estimate=cost(1e9 * n),
    )(tp, hidden, weight)


def total_kernel(a0, b0, c0, a1, b1, c1, out_ref):
    n = HALF_EXPERTS * SLOT_ROWS
    out_ref[:n] = (a0[...].astype(f32) + b0[...].astype(f32) + c0[...].astype(f32)).astype(bf16)
    out_ref[n:] = (a1[...].astype(f32) + b1[...].astype(f32) + c1[...].astype(f32)).astype(bf16)


def total_of(*args):
    return pl.pallas_call(
        total_kernel,
        out_shape=jax.ShapeDtypeStruct((EXPERTS * SLOT_ROWS, HALF), bf16),
        in_specs=whole(*[pltpu.VMEM] * 6),
        out_specs=whole(pltpu.VMEM)[0],
        name="total",
        compiler_params=params(8),
    )(*args)


def combine_kernel(index_ref, logits_ref, low_ref, out_ref):
    e = jnp.exp(logits_ref[...])
    weight = e / jnp.sum(e, axis=1, keepdims=True)
    columns = lax.broadcasted_iota(jnp.int32, (TOK, EXPERTS * SLOT_ROWS), 1)
    rows = low_ref[...]
    for h in range(2):
        total = None
        for k in range(2):
            at = index_ref[:, 2 * h + k : 2 * h + k + 1]
            pick = jnp.where(columns == at, 1.0, 0.0).astype(bf16)
            term = dot(pick, rows) * weight[:, k : k + 1]
            total = term if total is None else total + term
        out_ref[:, h * HALF : (h + 1) * HALF] = total.astype(bf16)


def combine(index, logits, rows):
    return pl.pallas_call(
        combine_kernel,
        out_shape=jax.ShapeDtypeStruct((TOK, GC), bf16),
        in_specs=whole(*[pltpu.VMEM] * 3),
        out_specs=whole(pltpu.VMEM)[0],
        name="combine",
        compiler_params=params(16),
    )(index, logits, rows)


RIM = 16
EXT = RIM + TOK


def squares_kernel(rim_ref, own_ref, out_ref):
    rim = rim_ref[...].astype(f32)
    own = own_ref[...].astype(f32)
    out_ref[:RIM] = jnp.broadcast_to(jnp.sum(rim * rim, axis=1, keepdims=True), (RIM, 128))
    out_ref[RIM:] = jnp.broadcast_to(jnp.sum(own * own, axis=1, keepdims=True), (TOK, 128))


def mixer_kernel(place_ref, squares_ref, rim_ref, own_ref, gain_ref, weight_ref, scale_ref, out_ref):
    group = place_ref[1]
    rows = jnp.concatenate([rim_ref[...], own_ref[...]], axis=0).astype(f32)
    normed = (rows * lax.rsqrt(squares_ref[:, :1] / D + EPS) * gain_ref[...]).astype(bf16).astype(f32)
    window = normed + pltpu.roll(normed, 1, 0)
    for level in range(1, 4):
        window = window + jnp.where(group >= level, pltpu.roll(window, 2**level, 0), 0.0)
    length = jnp.left_shift(jnp.int32(1), group + 1).astype(f32)
    position = (
        place_ref[0] * TOK + 1 + lax.broadcasted_iota(jnp.int32, (TOK, GC), 0)
    ).astype(f32)
    pooled = window[RIM:] / jnp.minimum(position, length)
    difference = (pooled - normed[RIM:]).astype(bf16)
    out_ref[...] = (dot(difference, weight_ref[...]) * scale_ref[...]).astype(bf16)


def rim_rows(tokens_a):
    peers = lax.axis_size("ep")
    return lax.ppermute(tokens_a[TOK - RIM :], "ep", [(i, i + 1) for i in range(peers - 1)])


def mixer(place, rim, tokens_a, gain, weight, scale):
    squares = pl.pallas_call(
        squares_kernel,
        out_shape=jax.ShapeDtypeStruct((EXT, 128), f32),
        in_specs=whole(*[pltpu.VMEM] * 2),
        out_specs=whole(pltpu.VMEM)[0],
        name="squares",
        compiler_params=params(4),
    )(rim, tokens_a)
    total = squares
    for step in (1, 3, 2):
        total = total + around(squares, step)
    return pl.pallas_call(
        mixer_kernel,
        out_shape=jax.ShapeDtypeStruct((TOK, GC), bf16),
        in_specs=whole(pltpu.SMEM, *[pltpu.VMEM] * 6),
        out_specs=whole(pltpu.VMEM)[0],
        name="mixer",
        compiler_params=params(8),
        cost_estimate=cost(5e9),
    )(place, total, rim, tokens_a, gain, weight, scale)


def around(x, step):
    return lax.ppermute(x, "tp", [(i, (i + step) % 4) for i in range(4)])


def shards(
    tokens_a,
    norm_gain_a,
    pool_weight,
    pool_scale,
    tokens_b,
    norm_gain_b,
    routes,
    route_logits,
    expert_gate,
    expert_up,
    expert_down,
):
    ep = lax.axis_index("ep").astype(jnp.int32)
    tp = lax.axis_index("tp").astype(jnp.int32)
    tp_at = tp[None]
    rim = rim_rows(tokens_a)
    packed, index = pack(tp_at, tokens_b, norm_gain_b[None, :], routes.T)
    packed, rim = lax.optimization_barrier((packed, rim))
    received = lax.all_to_all(
        packed.reshape(EXPERTS, SLOT_ROWS, HALF), "ep", 0, 0, tiled=True
    ).reshape(2, HALF_EXPERTS * SLOT_ROWS, HALF)
    mixed_a = mixer(
        jnp.stack([ep, tp]), rim, tokens_a, norm_gain_a[None], pool_weight[0], pool_scale[None]
    )
    received, mixed_a = lax.optimization_barrier((received, mixed_a))
    a, b = received[0], received[1]
    before_a, after_b = around(a, 1), around(b, 3)
    before_b, after_a = around(b, 1), around(a, 3)
    far_a, far_b = around(before_a, 1), around(after_b, 3)
    gate, up, down_w = expert_gate[0], expert_up[0], expert_down[0]
    gate_acc, up_acc = own_share(tp_at, gate, up, a, b)
    gate_acc, up_acc = near_share(
        tp_at, gate, up, gate_acc, up_acc, before_a, before_b, after_a, after_b
    )
    hidden = far_share(tp_at, gate, up, gate_acc, up_acc, far_a, far_b)
    far1, far2 = down("down_far", (2,), tp_at, hidden, down_w)
    got_far1, got_far2 = around(far1, 1), around(far2, 3)
    next1, next2, prev1, prev2 = down("down_near", (1, 3), tp_at, hidden, down_w)
    from_before2, from_after1 = around(next2, 1), around(prev1, 3)
    own1, own2 = down("down_own", (0,), tp_at, hidden, down_w)
    plus = lambda *xs: functools.reduce(jnp.add, [x.astype(f32) for x in xs]).astype(bf16)
    from_before1 = around(plus(next1, got_far1), 1)
    from_after2 = around(plus(prev2, got_far2), 3)
    summed = total_of(own1, from_before1, from_after1, own2, from_before2, from_after2)
    returned = lax.all_to_all(
        summed.reshape(EXPERTS, SLOT_ROWS, HALF), "ep", 0, 0, tiled=True
    ).reshape(EXPERTS * SLOT_ROWS, HALF)
    moe_out = combine(index.T, route_logits, returned)
    return mixed_a, moe_out


def solution(mesh):
    placed = (
        P("ep", "tp"),
        P("tp"),
        P("tp", None, None),
        P("tp"),
        P("ep", None),
        P(),
        P("ep", None),
        P("ep", None),
        P("ep", None, "tp"),
        P("ep", None, "tp"),
        P("ep", "tp", None),
    )
    return jax.shard_map(
        shards,
        mesh=mesh,
        in_specs=placed,
        out_specs=(P("ep", "tp"), P("ep", "tp")),
        check_vma=False,
    )
```

```python
import functools

import jax
import jax.numpy as jnp
from jax import lax
from jax.experimental import pallas as pl
from jax.experimental.pallas import tpu as pltpu
from jax.sharding import PartitionSpec as P


D = 2048
EPS = 1e-06
EXPERTS = 64
TOK = 256
GC = 512
FF_PART = 896
HALF = 256
SLOT_ROWS = 24
HALF_EXPERTS = EXPERTS // 2


PACK_MIB = 60
f32 = jnp.float32
bf16 = jnp.bfloat16


def whole(*names):
    return [pl.BlockSpec(memory_space=n) for n in names]


def dot(a, b):
    return jnp.dot(a, b, preferred_element_type=f32)


def pack_kernel(tp_ref, routes_ref, tokens_hbm, gain_hbm, out_ref, index_ref, tokens_ref, gain_ref, sem):
    tokens_in = pltpu.make_async_copy(tokens_hbm, tokens_ref, sem.at[0])
    gain_in = pltpu.make_async_copy(gain_hbm, gain_ref, sem.at[1])
    tokens_in.start()
    gain_in.start()
    share = tp_ref[0]
    expert_rows = lax.broadcasted_iota(jnp.int32, (EXPERTS, TOK), 0)
    earlier = (
        lax.broadcasted_iota(jnp.int32, (TOK, TOK), 0) < lax.broadcasted_iota(jnp.int32, (TOK, TOK), 1)
    ).astype(f32).astype(bf16)
    first = jnp.zeros((EXPERTS, 1), f32)
    lows, highs = [], []
    for k in range(2):
        chosen = routes_ref[k : k + 1, :]
        onehot = (expert_rows == chosen).astype(f32)
        count = dot(onehot.astype(bf16), earlier) + first
        slot = jnp.sum(onehot * count, axis=0, keepdims=True).astype(jnp.int32)
        first = first + jnp.sum(onehot, axis=1, keepdims=True)
        base = chosen * SLOT_ROWS
        lows.append(base + jnp.where(slot < 8, slot, slot + 8))
        highs.append(base + jnp.where(slot < 8, slot + 8, slot + 12))
    index_ref[...] = jnp.concatenate([*lows, *highs], axis=0)
    rows = lax.broadcasted_iota(jnp.int32, (EXPERTS * SLOT_ROWS, TOK), 0)
    low = jnp.where((rows == lows[0]) | (rows == lows[1]), 1.0, 0.0).astype(bf16)
    high = jnp.where((rows == highs[0]) | (rows == highs[1]), 1.0, 0.0).astype(bf16)
    tokens_in.wait()
    gain_in.wait()
    x = tokens_ref[...].astype(f32)
    mean = jnp.sum(x * x, axis=1, keepdims=True) / D
    start = pl.multiple_of(share * GC, GC)
    own = tokens_ref[:, pl.ds(start, GC)].astype(f32)
    normed = (own * lax.rsqrt(mean + EPS) * gain_ref[:, pl.ds(start, GC)]).astype(bf16)
    out_ref[...] = (dot(low, normed[:, :HALF]) + dot(high, normed[:, HALF:])).astype(bf16)


def pack(tp, routes, tokens_b, gain):
    return pl.pallas_call(
        pack_kernel,
        out_shape=(
            jax.ShapeDtypeStruct((EXPERTS * SLOT_ROWS, HALF), bf16),
            jax.ShapeDtypeStruct((4, TOK), jnp.int32),
        ),
        in_specs=whole(pltpu.SMEM, pltpu.VMEM, pl.ANY, pl.ANY),
        out_specs=tuple(whole(pltpu.VMEM, pltpu.VMEM)),
        scratch_shapes=[
            pltpu.VMEM((TOK, D), bf16),
            pltpu.VMEM((1, D), f32),
            pltpu.SemaphoreType.DMA((2,)),
        ],
        name="pack",
        compiler_params=params(PACK_MIB),
    )(tp, routes, tokens_b, gain)


HALF_ROWS = HALF_EXPERTS * 12
MAIN = HALF_EXPERTS * 8
MIX = HALF_EXPERTS * 4


def picker(n_out, n_in, group_out, group_in, offset):
    r = lax.broadcasted_iota(jnp.int32, (n_out, n_in), 0)
    c = lax.broadcasted_iota(jnp.int32, (n_out, n_in), 1)
    if group_out < group_in:
        hit = (r // group_out) * group_in + r % group_out + offset == c
    else:
        hit = (c // group_in) * group_out + c % group_in + offset == r
    return hit.astype(f32).astype(bf16)


def rows_of(ref):
    a = ref[...].reshape(HALF_EXPERTS, SLOT_ROWS, HALF)
    main = jnp.concatenate([a[:, 0:8].reshape(MAIN, HALF), a[:, 8:16].reshape(MAIN, HALF)], axis=1)
    mixed = a[:, 16:24].reshape(MAIN, HALF)
    low = dot(picker(MIX, MAIN, 4, 8, 0), mixed).astype(bf16)
    high = dot(picker(MIX, MAIN, 4, 8, 4), mixed).astype(bf16)
    return jnp.concatenate([main, jnp.concatenate([low, high], axis=1)], axis=0)


def store_rows(ref, rows):
    main, mix = rows[:MAIN], rows[MAIN:]
    tail = dot(picker(MAIN, MIX, 8, 4, 0), mix[:, :HALF]) + dot(picker(MAIN, MIX, 8, 4, 4), mix[:, HALF:])
    pieces = [
        main[:, :HALF].reshape(HALF_EXPERTS, 8, HALF),
        main[:, HALF:].reshape(HALF_EXPERTS, 8, HALF),
        tail.astype(bf16).reshape(HALF_EXPERTS, 8, HALF),
    ]
    ref[...] = jnp.concatenate(pieces, axis=1).reshape(HALF_EXPERTS * SLOT_ROWS, HALF)


def params(mib):
    return pltpu.CompilerParams(vmem_limit_bytes=mib * 1024 * 1024)


def cost(flops):
    return pl.CostEstimate(flops=int(flops), bytes_accessed=1 << 20, transcendentals=0)


PIECE = jax.ShapeDtypeStruct((HALF_EXPERTS * SLOT_ROWS, HALF), bf16)
ACC = jax.ShapeDtypeStruct((2 * HALF_ROWS, FF_PART), f32)


def half_span(h):
    return pl.ds(h * HALF_ROWS, HALF_ROWS)


def slab(tp_ref, step):
    return pl.ds(pl.multiple_of(((tp_ref[0] + step) % 4) * GC, GC), GC)


def own_share_kernel(tp_ref, gate_ref, up_ref, x0_ref, x1_ref, gate_acc, up_acc):
    at = slab(tp_ref, 0)
    for h, x_ref in enumerate((x0_ref, x1_ref)):
        x = rows_of(x_ref)
        gate_acc[half_span(h)] = dot(x, gate_ref[at, :])
        up_acc[half_span(h)] = dot(x, up_ref[at, :])


def own_share(*args):
    return pl.pallas_call(
        own_share_kernel,
        out_shape=(ACC,) * 2,
        in_specs=whole(pltpu.SMEM, *[pltpu.VMEM] * 4),
        out_specs=tuple(whole(*[pltpu.VMEM] * 2)),
        name="own_share",
        compiler_params=params(24),
        cost_estimate=cost(5e9),
    )(*args)


def near_share_kernel(tp_ref, gate_ref, up_ref, gate_in, up_in, x00, x01, x10, x11, gate_acc, up_acc):
    before, after = slab(tp_ref, 3), slab(tp_ref, 1)
    for h, (xa, xb) in enumerate(((x00, x10), (x01, x11))):
        a, b = rows_of(xa), rows_of(xb)
        span = half_span(h)
        gate_acc[span] = gate_in[span] + (dot(a, gate_ref[before, :]) + dot(b, gate_ref[after, :]))
        up_acc[span] = up_in[span] + (dot(a, up_ref[before, :]) + dot(b, up_ref[after, :]))


def near_share(*args):
    return pl.pallas_call(
        near_share_kernel,
        out_shape=(ACC,) * 2,
        in_specs=whole(pltpu.SMEM, *[pltpu.VMEM] * 8),
        out_specs=tuple(whole(*[pltpu.VMEM] * 2)),
        input_output_aliases={3: 0, 4: 1},
        name="near_share",
        compiler_params=params(24),
        cost_estimate=cost(5e9),
    )(*args)


def far_share_kernel(tp_ref, gate_ref, up_ref, gate_in, up_in, x0, x1, hidden_ref):
    at = slab(tp_ref, 2)
    for h, x_ref in enumerate((x0, x1)):
        x = rows_of(x_ref)
        span = half_span(h)
        g = gate_in[span] + dot(x, gate_ref[at, :])
        u = up_in[span] + dot(x, up_ref[at, :])
        hidden_ref[span] = (g / (1.0 + jnp.exp(-g)) * u).astype(bf16)


def far_share(*args):
    return pl.pallas_call(
        far_share_kernel,
        out_shape=jax.ShapeDtypeStruct((2 * HALF_ROWS, FF_PART), bf16),
        in_specs=whole(pltpu.SMEM, *[pltpu.VMEM] * 6),
        out_specs=whole(pltpu.VMEM)[0],
        name="far_share",
        compiler_params=params(24),
        cost_estimate=cost(5e9),
    )(*args)


def down_kernel(steps, tp_ref, hidden_ref, down_ref, *out_refs):
    for i, step in enumerate(steps):
        weight = down_ref[:, slab(tp_ref, step)]
        for h in range(2):
            store_rows(out_refs[2 * i + h], dot(hidden_ref[half_span(h)], weight).astype(bf16))


def down(steps, tp, hidden, weight):
    n = len(steps)
    return pl.pallas_call(
        functools.partial(down_kernel, steps),
        out_shape=(PIECE,) * (2 * n),
        in_specs=whole(pltpu.SMEM, *[pltpu.VMEM] * 2),
        out_specs=tuple(whole(*[pltpu.VMEM] * (2 * n))),
        compiler_params=params(16),
        cost_estimate=cost(1e9 * n),
    )(tp, hidden, weight)


def total_kernel(a0, b0, c0, a1, b1, c1, out_ref):
    n = HALF_EXPERTS * SLOT_ROWS
    out_ref[:n] = (a0[...].astype(f32) + b0[...].astype(f32) + c0[...].astype(f32)).astype(bf16)
    out_ref[n:] = (a1[...].astype(f32) + b1[...].astype(f32) + c1[...].astype(f32)).astype(bf16)


def total_of(*args):
    return pl.pallas_call(
        total_kernel,
        out_shape=jax.ShapeDtypeStruct((EXPERTS * SLOT_ROWS, HALF), bf16),
        in_specs=whole(*[pltpu.VMEM] * 6),
        out_specs=whole(pltpu.VMEM)[0],
        name="total",
        compiler_params=params(8),
    )(*args)


def combine_kernel(index_ref, logits_ref, low_ref, out_ref):
    e = jnp.exp(logits_ref[...])
    weight = e / jnp.sum(e, axis=1, keepdims=True)
    columns = lax.broadcasted_iota(jnp.int32, (TOK, EXPERTS * SLOT_ROWS), 1)
    rows = low_ref[...]
    for h in range(2):
        total = None
        for k in range(2):
            at = index_ref[:, 2 * h + k : 2 * h + k + 1]
            pick = jnp.where(columns == at, 1.0, 0.0).astype(bf16)
            term = dot(pick, rows) * weight[:, k : k + 1]
            total = term if total is None else total + term
        out_ref[:, h * HALF : (h + 1) * HALF] = total.astype(bf16)


def combine(index, logits, rows):
    return pl.pallas_call(
        combine_kernel,
        out_shape=jax.ShapeDtypeStruct((TOK, GC), bf16),
        in_specs=whole(*[pltpu.VMEM] * 3),
        out_specs=whole(pltpu.VMEM)[0],
        name="combine",
        compiler_params=params(16),
    )(index, logits, rows)


RIM = 16
EXT = RIM + TOK


def squares_kernel(rim_ref, own_ref, out_ref):
    rim = rim_ref[...].astype(f32)
    own = own_ref[...].astype(f32)
    out_ref[:RIM] = jnp.broadcast_to(jnp.sum(rim * rim, axis=1, keepdims=True), (RIM, 128))
    out_ref[RIM:] = jnp.broadcast_to(jnp.sum(own * own, axis=1, keepdims=True), (TOK, 128))


def mixer_kernel(place_ref, squares_ref, rim_ref, own_ref, gain_ref, weight_ref, scale_ref, out_ref):
    group = place_ref[1]
    rows = jnp.concatenate([rim_ref[...], own_ref[...]], axis=0).astype(f32)
    normed = (rows * lax.rsqrt(squares_ref[:, :1] / D + EPS) * gain_ref[...]).astype(bf16).astype(f32)
    window = normed + pltpu.roll(normed, 1, 0)
    for level in range(1, 4):
        window = window + jnp.where(group >= level, pltpu.roll(window, 2**level, 0), 0.0)
    length = jnp.left_shift(jnp.int32(1), group + 1).astype(f32)
    position = (
        place_ref[0] * TOK + 1 + lax.broadcasted_iota(jnp.int32, (TOK, GC), 0)
    ).astype(f32)
    pooled = window[RIM:] / jnp.minimum(position, length)
    difference = (pooled - normed[RIM:]).astype(bf16)
    out_ref[...] = (dot(difference, weight_ref[...]) * scale_ref[...]).astype(bf16)


def rim_rows(tokens_a):
    peers = lax.axis_size("ep")
    return lax.ppermute(tokens_a[TOK - RIM :], "ep", [(i, i + 1) for i in range(peers - 1)])


def mixer(place, rim, tokens_a, gain, weight, scale):
    squares = pl.pallas_call(
        squares_kernel,
        out_shape=jax.ShapeDtypeStruct((EXT, 128), f32),
        in_specs=whole(*[pltpu.VMEM] * 2),
        out_specs=whole(pltpu.VMEM)[0],
        name="squares",
        compiler_params=params(4),
    )(rim, tokens_a)
    total = squares
    for step in (1, 3, 2):
        total = total + around(squares, step)
    return pl.pallas_call(
        mixer_kernel,
        out_shape=jax.ShapeDtypeStruct((TOK, GC), bf16),
        in_specs=whole(pltpu.SMEM, *[pltpu.VMEM] * 6),
        out_specs=whole(pltpu.VMEM)[0],
        name="mixer",
        compiler_params=params(8),
        cost_estimate=cost(5e9),
    )(place, total, rim, tokens_a, gain, weight, scale)


def around(x, step):
    return lax.ppermute(x, "tp", [(i, (i + step) % 4) for i in range(4)])


def shards(
    tokens_a,
    norm_gain_a,
    pool_weight,
    pool_scale,
    tokens_b,
    norm_gain_b,
    routes,
    route_logits,
    expert_gate,
    expert_up,
    expert_down,
):
    ep = lax.axis_index("ep").astype(jnp.int32)
    tp = lax.axis_index("tp").astype(jnp.int32)
    tp_at = tp[None]
    packed, index = pack(tp_at, routes.T, tokens_b, norm_gain_b[None, :])
    received = lax.all_to_all(
        packed.reshape(EXPERTS, SLOT_ROWS, HALF), "ep", 0, 0, tiled=True
    ).reshape(2, HALF_EXPERTS * SLOT_ROWS, HALF)
    received, tokens_a = lax.optimization_barrier((received, tokens_a))
    a, b = received[0], received[1]
    before_a, after_b = around(a, 1), around(b, 3)
    before_b, after_a = around(b, 1), around(a, 3)
    far_a, far_b = around(before_a, 1), around(after_b, 3)
    rim = rim_rows(tokens_a)
    gate, up, down_w = expert_gate[0], expert_up[0], expert_down[0]
    gate_acc, up_acc = own_share(tp_at, gate, up, a, b)
    gate_acc, up_acc = near_share(
        tp_at, gate, up, gate_acc, up_acc, before_a, before_b, after_a, after_b
    )
    hidden = far_share(tp_at, gate, up, gate_acc, up_acc, far_a, far_b)
    far1, far2 = down((2,), tp_at, hidden, down_w)
    got_far1, got_far2 = around(far1, 1), around(far2, 3)
    next1, next2, prev1, prev2 = down((1, 3), tp_at, hidden, down_w)
    from_before2, from_after1 = around(next2, 1), around(prev1, 3)
    own1, own2 = down((0,), tp_at, hidden, down_w)
    plus = lambda *xs: functools.reduce(jnp.add, [x.astype(f32) for x in xs]).astype(bf16)
    from_before1 = around(plus(next1, got_far1), 1)
    from_after2 = around(plus(prev2, got_far2), 3)
    summed = total_of(own1, from_before1, from_after1, own2, from_before2, from_after2)
    summed, rim = lax.optimization_barrier((summed, rim))
    returned = lax.all_to_all(
        summed.reshape(EXPERTS, SLOT_ROWS, HALF), "ep", 0, 0, tiled=True
    ).reshape(EXPERTS * SLOT_ROWS, HALF)
    mixed_a = mixer(
        jnp.stack([ep, tp]), rim, tokens_a, norm_gain_a[None], pool_weight[0], pool_scale[None]
    )
    returned, mixed_a = lax.optimization_barrier((returned, mixed_a))
    moe_out = combine(index.T, route_logits, returned)
    return mixed_a, moe_out


def solution(mesh):
    placed = (
        P("ep", "tp"),
        P("tp"),
        P("tp", None, None),
        P("tp"),
        P("ep", None),
        P(),
        P("ep", None),
        P("ep", None),
        P("ep", None, "tp"),
        P("ep", None, "tp"),
        P("ep", "tp", None),
    )
    return jax.shard_map(
        shards,
        mesh=mesh,
        in_specs=placed,
        out_specs=(P("ep", "tp"), P("ep", "tp")),
        check_vma=False,
    )
```
